32 devices in a mesh: sp: 16 (over z, x, core), tp: 2 (over y).
Axes of the slice: x: 2, y: 2, z: 4, core: 2. Of those that a mesh axis runs over, the one named last changes fastest.
Arguments:
- value_rows: bfloat16 [16384, 1024], P('sp', 'tp'), may hold values from -6 to 6
- gate_rows: bfloat16 [16384, 1024], P('sp', 'tp'), may hold values from -6 to 6
- conv_taps: bfloat16 [31, 1024], P(None, 'tp'), may hold values from -1 to 1
- norm_gain: float32 [1024], P('tp'), may hold values from 0.1 to 1.9
- point_weight: bfloat16 [1024, 1024], P(None, 'tp'), may hold values from -0.1875 to 0.1875
- out_grad: bfloat16 [16384, 1024], P('sp', 'tp'), may hold values from -6 to 6
Outputs:
- value_grad: bfloat16 [16384, 1024], P('sp', 'tp')
- gate_grad: bfloat16 [16384, 1024], P('sp', 'tp')
- taps_grad: float32 [31, 1024], P(None, 'tp')
- gain_grad: float32 [1024], P('tp')
- weight_grad: float32 [1024, 1024], P('sp', 'tp')
The draws below stay inside these ranges and needn't reach their ends.
All inputs are finite; a program needn't handle non-finite values.
Results may differ from the reference program's by a relative error of at most 0.0051.
Values may be sent and summed in bfloat16 or wider, within the bound.
A program may use at most 128 MiB of HBM per device.

```python
import jax
import jax.numpy as jnp
from jax import lax

C = 1024
GROUP = 64
KW = 31
HALF = 15
TOK_DEV = 1024
TOKENS = 16384


def raised(array, key, source, target, blocks, factor):
    def block_of(dim):
        return (jnp.arange(array.shape[dim]) // (array.shape[dim] // blocks)).reshape((-1,) + (1,) * (array.ndim - 1 - dim))

    near = jax.random.permutation(key, blocks)[block_of(target)]
    second = (block_of(target) + blocks // 2) % blocks
    return jnp.where((block_of(source) == near) | (block_of(source) == second), factor * array, array)


def block_levels(rng, dims, cuts, least, largest):
    def one(position, shards_of):
        draws = jax.random.uniform(jax.random.fold_in(jax.random.fold_in(rng, 6), position), (shards_of,), jnp.float32, least / len(cuts), largest / len(cuts))
        return jnp.repeat(jnp.exp(draws), dims[position] // shards_of).reshape((-1,) + (1,) * (len(dims) - position - 1))

    loudness = one(*cuts[0])
    for cut in cuts[1:]:
        loudness = loudness * one(*cut)
    return loudness


def gaussian(key, shape, deviation, most, pieces=(), held_as=jnp.bfloat16):
    result = jax.random.normal(key, shape, jnp.float32) * deviation
    if len(pieces) > 0:
        result = block_levels(key, shape, pieces, -0.22, 0.18) * result
    return jnp.clip(result, min=-most, max=most).astype(held_as)


def heavy_noise(stream_key, dims, deviation, most, shards, heavy, held_as=jnp.bfloat16):
    drawn = deviation * jax.random.normal(stream_key, dims, jnp.float32)
    if shards:
        drawn = drawn * block_levels(stream_key, dims, shards, -0.22, 0.18)
    return jnp.clip(raised(drawn, jax.random.fold_in(stream_key, 3), *heavy), -most, most).astype(held_as)


def setup_inputs(seed: int = 0) -> dict:
    splits = jax.random.split(jax.random.key(seed), 7)
    return {
        "value_rows": gaussian(splits[0], (TOKENS, C), 1.0, 6.0, ((0, 16), (1, 2))),
        "gate_rows": gaussian(splits[1], (TOKENS, C), 1.0, 6.0, ((0, 16), (1, 2))),
        "conv_taps": gaussian(splits[2], (KW, C), KW ** -0.5, 1.0, ((1, 2),)),
        "norm_gain": jnp.clip(1.0 + 0.18 * jax.random.normal(splits[3], (C,), jnp.float32), 0.1, 1.9),
        "point_weight": gaussian(splits[4], (C, C), C ** -0.5, 0.1875, ((1, 2),)),
        "out_grad": heavy_noise(splits[5], (TOKENS, C), 1.0, 6.0, ((0, 16), (1, 2)), (0, 1, 16, 2.0)),
    }


EPS = 1e-06

def reference(value_rows, gate_rows, conv_taps, norm_gain, point_weight, out_grad):
    total_rows = value_rows.shape[0]
    block_rows = TOK_DEV
    block_count = total_rows // block_rows
    groups = C // GROUP
    gate_sig_all = jax.nn.sigmoid(gate_rows.astype(jnp.float32))
    gated_all = (value_rows.astype(jnp.float32) * gate_sig_all).astype(jnp.bfloat16)
    gated_pad = jnp.pad(gated_all, ((2 * HALF, 2 * HALF), (0, 0)))
    grad_pad = jnp.pad(out_grad, ((HALF, HALF), (0, 0)))
    taps_f = conv_taps.astype(jnp.float32)
    gain_g = norm_gain.astype(jnp.float32).reshape(groups, GROUP)
    extent = block_rows + 2 * HALF

    def one_block(carry, block_index):
        taps_acc, gain_acc, weight_acc = carry
        start = (block_index * block_rows).astype(jnp.int32)
        gated_wide = lax.dynamic_slice_in_dim(gated_pad, start, block_rows + 4 * HALF, 0)
        cotangent = lax.dynamic_slice_in_dim(grad_pad, start, extent, 0)
        value_f = lax.dynamic_slice_in_dim(value_rows, start, block_rows, 0).astype(jnp.float32)
        gate_sig = lax.dynamic_slice_in_dim(gate_sig_all, start, block_rows, 0)
        convolved = jnp.zeros((extent, C), jnp.float32)
        for tap_index in range(KW):
            convolved = convolved + taps_f[tap_index] * gated_wide[tap_index:tap_index + extent].astype(jnp.float32)
        grouped = convolved.reshape(extent, groups, GROUP)
        group_mean = lax.optimization_barrier(jnp.mean(grouped, axis=-1, keepdims=True))
        centred = grouped - group_mean
        inv_std = lax.rsqrt(lax.optimization_barrier(jnp.mean(centred * centred, axis=-1, keepdims=True)) + EPS)
        unit_conv = centred * inv_std
        pre_act = unit_conv * gain_g
        act_sig = jax.nn.sigmoid(pre_act)
        normed = (pre_act * act_sig).astype(jnp.bfloat16).reshape(extent, C)
        normed_grad = jnp.dot(cotangent, point_weight, preferred_element_type=jnp.float32).reshape(extent, groups, GROUP)
        own_grad = cotangent[HALF:HALF + block_rows]
        own_normed = normed[HALF:HALF + block_rows]
        weight_part = lax.dot_general(own_grad, own_normed, (((0,), (0,)), ((), ())), preferred_element_type=jnp.float32)
        act_grad = normed_grad * act_sig * (1.0 + pre_act * (1.0 - act_sig))
        gain_part = lax.optimization_barrier(jnp.sum((act_grad * unit_conv)[HALF:HALF + block_rows], axis=0)).reshape(C)
        hat_grad = act_grad * gain_g
        conv_grad = inv_std * (hat_grad - lax.optimization_barrier(jnp.mean(hat_grad, axis=-1, keepdims=True)) - unit_conv * lax.optimization_barrier(jnp.mean(hat_grad * unit_conv, axis=-1, keepdims=True)))
        conv_grad = conv_grad.reshape(extent, C)
        own_conv = conv_grad[HALF:HALF + block_rows]
        taps_part = jnp.stack([lax.optimization_barrier(jnp.sum(own_conv * gated_wide[HALF + tap_index:HALF + tap_index + block_rows].astype(jnp.float32), axis=0)) for tap_index in range(KW)])
        gated_grad = jnp.zeros((block_rows, C), jnp.float32)
        for tap_index in range(KW):
            lower = 2 * HALF - tap_index
            gated_grad = gated_grad + taps_f[tap_index] * conv_grad[lower:lower + block_rows]
        value_grad = (gated_grad * gate_sig).astype(jnp.bfloat16)
        gate_grad = (gated_grad * value_f * gate_sig * (1.0 - gate_sig)).astype(jnp.bfloat16)
        return ((taps_acc + taps_part, gain_acc + gain_part, weight_acc + weight_part), (value_grad, gate_grad))
    init = (jnp.zeros((KW, C), jnp.float32), jnp.zeros((C,), jnp.float32), jnp.zeros((C, C), jnp.float32))
    sums, blocks = lax.scan(one_block, init, jnp.arange(block_count, dtype=jnp.int32))
    taps_grad, gain_grad, weight_grad = sums
    value_grad = blocks[0].reshape(total_rows, C)
    gate_grad = blocks[1].reshape(total_rows, C)
    return (value_grad, gate_grad, taps_grad, gain_grad, weight_grad)
```

```python
import functools

import jax
import jax.numpy as jnp
from jax import lax
from jax.experimental import pallas as pl
from jax.experimental.pallas import tpu as pltpu
from jax.sharding import PartitionSpec as P

GROUP = 64
EPS = 1e-06
LANE = 128
EDGE = 16
F32, BF16 = jnp.float32, jnp.bfloat16


def sigmoid(x):
    return 0.5 * jnp.tanh(0.5 * x) + 0.5


def divisor(total, *choices):
    for choice in choices:
        if total % choice == 0:
            return choice
    return total


def group_matrix():
    row = lax.broadcasted_iota(jnp.int32, (2 * LANE, LANE), 0)
    col = lax.broadcasted_iota(jnp.int32, (2 * LANE, LANE), 1)
    same = lax.rem(row, LANE) // GROUP == col // GROUP
    return jnp.where(same, 1.0 / GROUP, 0.0).astype(BF16)


def group_mean(x, matrix):
    high = x.astype(BF16)
    low = (x - high.astype(F32)).astype(BF16)
    return jnp.dot(jnp.concatenate([high, low], axis=1), matrix, preferred_element_type=F32)


def lanes(c):
    return pl.ds(pl.multiple_of(c * LANE, LANE), LANE)


def forward(value, gate, vlo, vhi, glo, ghi, taps, gain, gated, unit, inv, normed):
    rows, chans = value.shape
    tiles = chans // LANE
    kw = taps.shape[1]
    extent = unit.shape[1]
    matrix = group_matrix()

    def gate_tile(c, _):
        def put(v_ref, g_ref, src, n, dst):
            v = v_ref[pl.ds(src, n), lanes(c)].astype(F32)
            g = g_ref[pl.ds(src, n), lanes(c)].astype(F32)
            gated[c, pl.ds(dst, n), :] = (v * sigmoid(g)).astype(BF16).astype(F32)

        put(vlo, glo, 0, 2 * EDGE, 0)
        put(vhi, ghi, 0, 2 * EDGE, rows + 2 * EDGE)
        step = divisor(rows, 256, 32)

        def chunk(r, _):
            at = pl.multiple_of(r * step, step)
            put(value, gate, at, step, pl.multiple_of(at + 2 * EDGE, 8))
            return 0

        lax.fori_loop(0, rows // step, chunk, 0)

        cstep = divisor(extent, 96, 32)

        def conv(r, _):
            at = r * cstep
            acc = jnp.zeros((cstep, LANE), F32)
            for k in range(kw):
                acc += taps[c, pl.ds(k, 1), :] * gated[c, pl.ds(at + (k + 2 * EDGE - EDGE - kw // 2), cstep), :]
            unit[c, pl.ds(pl.multiple_of(at, 8), cstep), :] = acc
            return 0

        lax.fori_loop(0, extent // cstep, conv, 0)

        nstep = divisor(extent, 352, 32)

        def norm(r, _):
            at = pl.multiple_of(r * nstep, 8)
            x = unit[c, pl.ds(at, nstep), :]
            centred = x - group_mean(x, matrix)
            rs = lax.rsqrt(group_mean(centred * centred, matrix) + EPS)
            inv[c, pl.ds(at, nstep), :] = rs
            unit[c, pl.ds(at, nstep), :] = centred * rs
            return 0

        lax.fori_loop(0, extent // nstep, norm, 0)

        def act(r, _):
            at = pl.multiple_of(r * step, step)
            p = unit[c, pl.ds(pl.multiple_of(at + EDGE, 8), step), :] * gain[:, lanes(c)]
            normed[pl.ds(at, step), lanes(c)] = (p * sigmoid(p)).astype(BF16)
            return 0

        lax.fori_loop(0, rows // step, act, 0)
        return 0

    lax.fori_loop(0, tiles, gate_tile, 0)


def middle(grad, others, elo, ehi, weight, unit, inv, normed, gain, dconv, gain_part, wpart):
    rows, chans = grad.shape
    tiles = chans // LANE
    peers = others.shape[0] + 1
    me = lax.axis_index("tp")
    matrix = group_matrix()
    step = divisor(rows, 256, 32)
    gain_part[...] = jnp.zeros_like(gain_part)

    def owner(j):
        return pl.ds(pl.multiple_of(lax.rem(me + j, peers) * chans, chans), chans)

    def finish(ng, at, n, own):
        for c in range(tiles):
            g = gain[:, c * LANE:(c + 1) * LANE]
            u = unit[c, pl.ds(at, n), :]
            p = u * g
            s = sigmoid(p)
            a = ng[:, c * LANE:(c + 1) * LANE] * s * (1.0 + p * (1.0 - s))
            au = a * u
            if own:
                gain_part[:, c * LANE:(c + 1) * LANE] += jnp.sum(au.reshape(n // 8, 8, LANE), axis=0)
            h = a * g
            hu = au * g
            dconv[c, pl.ds(at, n), :] = inv[c, pl.ds(at, n), :] * (
                h - group_mean(h, matrix) - u * group_mean(hu, matrix))

    for ref, at in ((elo, 0), (ehi, rows + EDGE)):
        ng = sum(jnp.dot(ref[j], weight[owner(j), :], preferred_element_type=F32) for j in range(peers))
        finish(ng, at, EDGE, False)

    def chunk(r, _):
        at = pl.multiple_of(r * step, step)
        ng = jnp.dot(grad[pl.ds(at, step), :], weight[owner(0), :], preferred_element_type=F32)
        for j in range(1, peers):
            ng += jnp.dot(others[j - 1, pl.ds(at, step), :], weight[owner(j), :], preferred_element_type=F32)
        finish(ng, pl.multiple_of(at + EDGE, 8), step, True)
        return 0

    lax.fori_loop(0, rows // step, chunk, 0)

    piece = divisor(chans, 256, 128)
    for j in range(peers):
        def cols(q, _):
            src = pl.ds(pl.multiple_of(q * piece, piece), piece)
            lhs = grad[:, src] if j == 0 else others[j - 1, :, src]
            out = lax.dot_general(lhs, normed[...], (((0,), (0,)), ((), ())), preferred_element_type=F32)
            base = lax.rem(me + j, peers) * chans
            wpart[pl.ds(pl.multiple_of(base + q * piece, piece), piece), :] = out
            return 0

        lax.fori_loop(0, chans // piece, cols, 0)


def taps_body(dconv, gated, sums):
    tiles, kw1 = sums.shape[0], sums.shape[1]
    kw = kw1 - 1
    rows = dconv.shape[1] - 2 * EDGE

    def tile(c, _):
        def chunk(r, accs):
            at = r * 16
            out = []
            d0 = dconv[c, pl.ds(pl.multiple_of(at + EDGE, 8), 8), :]
            d1 = dconv[c, pl.ds(pl.multiple_of(at + EDGE + 8, 8), 8), :]
            for k in range(kw):
                g0 = gated[c, pl.ds(at + (k + 2 * EDGE - kw // 2), 8), :]
                g1 = gated[c, pl.ds(at + (k + 2 * EDGE - kw // 2 + 8), 8), :]
                out.append(accs[k] + (d0 * g0 + d1 * g1))
            return tuple(out)

        accs = lax.fori_loop(0, rows // 16, chunk, tuple(jnp.zeros((8, LANE), F32) for _ in range(kw)))
        for k in range(kw):
            sums[c, pl.ds(k, 1), :] = jnp.sum(accs[k], axis=0, keepdims=True)
        return 0

    lax.fori_loop(0, tiles, tile, 0)


def taps_kernel(dconv, gated, gain_part, sums):
    taps_body(dconv, gated, sums)
    kw = sums.shape[1] - 1
    for c in range(sums.shape[0]):
        sums[c, pl.ds(kw, 1), :] = jnp.sum(gain_part[:, c * LANE:(c + 1) * LANE], axis=0, keepdims=True)


def backward(dconv, value, gate, taps, vgrad, ggrad):
    rows, chans = value.shape
    tiles = chans // LANE
    kw = taps.shape[1]
    step = divisor(rows, 64, 32)

    def tile(c, _):
        def chunk(r, _):
            at = pl.multiple_of(r * step, step)
            acc = jnp.zeros((step, LANE), F32)
            for k in range(kw):
                acc += taps[c, pl.ds(k, 1), :] * dconv[c, pl.ds(at + (EDGE + kw // 2 - k), step), :]
            s = sigmoid(gate[pl.ds(at, step), lanes(c)].astype(F32))
            v = value[pl.ds(at, step), lanes(c)].astype(F32)
            gs = acc * s
            vgrad[pl.ds(at, step), lanes(c)] = gs.astype(BF16)
            ggrad[pl.ds(at, step), lanes(c)] = (gs * v * (1.0 - s)).astype(BF16)
            return 0

        lax.fori_loop(0, rows // step, chunk, 0)
        return 0

    lax.fori_loop(0, tiles, tile, 0)


def call(body, outs, args, flops, bytes_accessed):
    return pl.pallas_call(
        body,
        out_shape=[jax.ShapeDtypeStruct(s, d) for s, d in outs],
        in_specs=[pl.BlockSpec(memory_space=pltpu.VMEM)] * len(args),
        out_specs=[pl.BlockSpec(memory_space=pltpu.VMEM)] * len(outs),
        compiler_params=pltpu.CompilerParams(vmem_limit_bytes=48 * 1024 * 1024),
        cost_estimate=pl.CostEstimate(flops=flops, bytes_accessed=bytes_accessed, transcendentals=0),
    )(*args)


def per_device(value, gate, conv_taps, norm_gain, point_weight, out_grad):
    rows, chans = value.shape
    kw = conv_taps.shape[0]
    tiles = chans // LANE
    n, peers = lax.axis_size("sp"), lax.axis_size("tp")
    extent = rows + 2 * EDGE
    up = [(i, i + 1) for i in range(n - 1)]
    down = [(j, i) for i, j in up]
    swap = [[((t + j) % peers, t) for t in range(peers)] for j in range(1, peers)]

    both = jnp.stack([value[-2 * EDGE:], gate[-2 * EDGE:]]), jnp.stack([value[:2 * EDGE], gate[:2 * EDGE]])
    lo = lax.ppermute(both[0], "sp", up)
    hi = lax.ppermute(both[1], "sp", down)
    edges = jnp.stack([out_grad[-EDGE:], out_grad[:EDGE]])
    elo = lax.ppermute(edges[0], "sp", up)
    ehi = lax.ppermute(edges[1], "sp", down)
    ends = jnp.stack([elo, ehi])
    ends = jnp.stack([ends] + [lax.ppermute(ends, "tp", s) for s in swap])
    others = jnp.stack([lax.ppermute(out_grad, "tp", s) for s in swap])
    taps = conv_taps.astype(F32).reshape(kw, tiles, LANE).transpose(1, 0, 2)
    gain = norm_gain.reshape(1, chans)

    big = rows * chans
    gated, unit, inv, normed = call(
        forward,
        [((tiles, rows + 4 * EDGE, LANE), F32), ((tiles, extent, LANE), F32), ((tiles, extent, LANE), F32), ((rows, chans), BF16)],
        [value, gate, lo[0], hi[0], lo[1], hi[1], taps, gain], 2 * kw * big, 20 * big)
    dconv, gain_part, wpart = call(
        middle,
        [((tiles, extent, LANE), F32), ((8, chans), F32), ((peers * chans, chans), F32)],
        [out_grad, others, ends[:, 0], ends[:, 1], point_weight, unit, inv, normed, gain], 8 * big * peers * chans // 2, 20 * big)
    (sums,) = call(taps_kernel, [((tiles, kw + 1, LANE), F32)], [dconv, gated, gain_part], 2 * kw * big, 20 * big)
    vgrad, ggrad = call(backward, [((rows, chans), BF16)] * 2, [dconv, value, gate, taps], 2 * kw * big, 20 * big)

    me = lax.axis_index("sp")
    w = wpart.reshape(n, peers * chans // n, chans)
    bit = 1
    while bit < n:
        pairs = [(i, i ^ bit) for i in range(n)]
        mine = (me // bit) % 2
        halves = w.reshape(w.shape[0] // 2, 2, *w.shape[1:])
        keep = lax.dynamic_index_in_dim(halves, mine, 1, keepdims=False)
        send = lax.dynamic_index_in_dim(halves, 1 - mine, 1, keepdims=False)
        w = keep + lax.ppermute(send.astype(BF16), "sp", pairs).astype(F32)
        sums = sums + lax.ppermute(sums, "sp", pairs)
        bit *= 2
    flat = sums.transpose(1, 0, 2).reshape(kw + 1, chans)
    return vgrad, ggrad, flat[:kw], flat[kw], w[0]


def solution(mesh):
    return jax.shard_map(
        per_device,
        mesh=mesh,
        in_specs=(P("sp", "tp"), P("sp", "tp"), P(None, "tp"), P("tp"), P(None, "tp"), P("sp", "tp")),
        out_specs=(P("sp", "tp"), P("sp", "tp"), P(None, "tp"), P("tp"), P("sp", "tp")),
        check_vma=False,
    )
```

```python
import functools

import jax
import jax.numpy as jnp
from jax import lax
from jax.experimental import pallas as pl
from jax.experimental.pallas import tpu as pltpu
from jax.sharding import PartitionSpec as P

GROUP = 64
EPS = 1e-06
LANE = 128
EDGE = 16
F32, BF16 = jnp.float32, jnp.bfloat16


def sigmoid(x):
    return 0.5 * jnp.tanh(0.5 * x) + 0.5


def divisor(total, *choices):
    for choice in choices:
        if total % choice == 0:
            return choice
    return total


def group_matrix():
    row = lax.broadcasted_iota(jnp.int32, (2 * LANE, LANE), 0)
    col = lax.broadcasted_iota(jnp.int32, (2 * LANE, LANE), 1)
    same = lax.rem(row, LANE) // GROUP == col // GROUP
    return jnp.where(same, 1.0 / GROUP, 0.0).astype(BF16)


def group_mean(x, matrix):
    high = x.astype(BF16)
    low = (x - high.astype(F32)).astype(BF16)
    return jnp.dot(jnp.concatenate([high, low], axis=1), matrix, preferred_element_type=F32)


def lanes(c):
    return pl.ds(pl.multiple_of(c * LANE, LANE), LANE)


def put_gated(gated, c, v, g, dst, n):
    gated[c, pl.ds(dst, n), :] = (v.astype(F32) * sigmoid(g.astype(F32))).astype(BF16).astype(F32)


def forward_tile(c, taps, gain, gated, unit, inv, normed, matrix):
    kw = taps.shape[1]
    extent = unit.shape[1]
    rows = normed.shape[0]
    cstep = divisor(extent, 96, 32)

    def conv(r, _):
        at = r * cstep
        acc = jnp.zeros((cstep, LANE), F32)
        for k in range(kw):
            acc += taps[c, pl.ds(k, 1), :] * gated[c, pl.ds(at + (k + EDGE - kw // 2), cstep), :]
        unit[c, pl.ds(pl.multiple_of(at, 8), cstep), :] = acc
        return 0

    lax.fori_loop(0, extent // cstep, conv, 0)
    nstep = divisor(extent, 352, 32)

    def norm(r, _):
        at = pl.multiple_of(r * nstep, 8)
        x = unit[c, pl.ds(at, nstep), :]
        centred = x - group_mean(x, matrix)
        rs = lax.rsqrt(group_mean(centred * centred, matrix) + EPS)
        inv[c, pl.ds(at, nstep), :] = rs
        unit[c, pl.ds(at, nstep), :] = centred * rs
        return 0

    lax.fori_loop(0, extent // nstep, norm, 0)
    step = divisor(rows, 256, 32)

    def act(r, _):
        at = pl.multiple_of(r * step, step)
        p = unit[c, pl.ds(pl.multiple_of(at + EDGE, 8), step), :] * gain[:, lanes(c)]
        normed[pl.ds(at, step), lanes(c)] = (p * sigmoid(p)).astype(BF16)
        return 0

    lax.fori_loop(0, rows // step, act, 0)


def act_to_conv(ng, at, n, own, unit, inv, gain, dconv, gain_part, matrix):
    for c in range(unit.shape[0]):
        g = gain[:, c * LANE:(c + 1) * LANE]
        u = unit[c, pl.ds(at, n), :]
        p = u * g
        s = sigmoid(p)
        a = ng[:, c * LANE:(c + 1) * LANE] * s * (1.0 + p * (1.0 - s))
        au = a * u
        if own:
            gain_part[:, c * LANE:(c + 1) * LANE] += jnp.sum(au.reshape(n // 8, 8, LANE), axis=0)
        h = a * g
        hu = au * g
        dconv[c, pl.ds(at, n), :] = inv[c, pl.ds(at, n), :] * (
            h - group_mean(h, matrix) - u * group_mean(hu, matrix))


def taps_tile(c, dconv, gated, gain_part, sums):
    kw = sums.shape[1] - 1
    rows = dconv.shape[1] - 2 * EDGE

    def chunk(r, accs):
        at = r * 16
        out = []
        d0 = dconv[c, pl.ds(pl.multiple_of(at + EDGE, 8), 8), :]
        d1 = dconv[c, pl.ds(pl.multiple_of(at + EDGE + 8, 8), 8), :]
        for k in range(kw):
            g0 = gated[c, pl.ds(at + (k + 2 * EDGE - kw // 2), 8), :]
            g1 = gated[c, pl.ds(at + (k + 2 * EDGE - kw // 2 + 8), 8), :]
            out.append(accs[k] + (d0 * g0 + d1 * g1))
        return tuple(out)

    accs = lax.fori_loop(0, rows // 16, chunk, tuple(jnp.zeros((8, LANE), F32) for _ in range(kw)))
    for k in range(kw):
        sums[c, pl.ds(k, 1), :] = jnp.sum(accs[k], axis=0, keepdims=True)
    sums[c, pl.ds(kw, 1), :] = jnp.sum(gain_part[:, lanes(c)], axis=0, keepdims=True)


def backward_tile(c, dconv, value, gate, taps, vgrad, ggrad):
    rows = value.shape[0]
    kw = taps.shape[1]
    step = divisor(rows, 64, 32)

    def chunk(r, _):
        at = pl.multiple_of(r * step, step)
        acc = jnp.zeros((step, LANE), F32)
        for k in range(kw):
            acc += taps[c, pl.ds(k, 1), :] * dconv[c, pl.ds(at + (EDGE + kw // 2 - k), step), :]
        s = sigmoid(gate[pl.ds(at, step), lanes(c)].astype(F32))
        v = value[pl.ds(at, step), lanes(c)].astype(F32)
        gs = acc * s
        vgrad[pl.ds(at, step), lanes(c)] = gs.astype(BF16)
        ggrad[pl.ds(at, step), lanes(c)] = (gs * v * (1.0 - s)).astype(BF16)
        return 0

    lax.fori_loop(0, rows // step, chunk, 0)


def loop(lo, hi, body):
    def one(i, _):
        body(i)
        return 0

    lax.fori_loop(lo, hi, one, 0)


def whole_kernel(n, peers, value, gate, taps, gain, weight, grad,
                 vgrad, ggrad, out_sums, wout,
                 gated, unit, inv, normed, dconv, gain_part, wpart, sums,
                 vhalo, ohalo, others, send1, recv1, send2, recv2, send3, recv3,
                 arecv1, arecv2, asum, arecv3, atotal,
                 vs, vr, os_, or_, gs, gr, ws, wr, ws3, wr3, as_, ar, as3, ar3):
    rows, chans = value.shape
    tiles = chans // LANE
    sp, tp = lax.axis_index("sp"), lax.axis_index("tp")
    group = recv3.shape[0] + 1
    half_tiles = tiles // 2
    b0, b1, zz = lax.rem(sp, 2), lax.rem(sp // 2, 2), sp // 4
    left, right = lax.rem(sp + n - 1, n), lax.rem(sp + 1, n)
    mate0 = sp + 1 - 2 * b0
    mate1 = sp + 2 - 4 * b1

    def zmate(d):
        return lax.rem(sp + 4 * d, n)

    def tmate(j):
        return lax.rem(tp + peers - j, peers)

    def remote(src, dst, s, r, to):
        return pltpu.make_async_remote_copy(
            src_ref=src, dst_ref=dst, send_sem=s, recv_sem=r, device_id=to,
            device_id_type=pl.DeviceIdType.MESH)

    barrier = pltpu.get_barrier_semaphore()
    friends = [(left, tmate(j)) for j in range(peers)] + [(right, tmate(j)) for j in range(peers)]
    friends += [(sp, tmate(j)) for j in range(1, peers)] + [(mate0, tp), (mate1, tp)]
    friends += [(zmate(d), tp) for d in range(1, group)]
    for friend in friends:
        pl.semaphore_signal(barrier, inc=1, device_id=friend, device_id_type=pl.DeviceIdType.MESH)
    pl.semaphore_wait(barrier, len(friends))

    wide = 2 * EDGE
    pending = []
    halos = []
    for side, (start, to) in enumerate(((rows - wide, right), (0, left))):
        for i, ref in enumerate((value, gate)):
            halos.append(remote(ref.at[pl.ds(start, wide)], vhalo.at[side, i], vs.at[side, i], vr.at[side, i], (to, tp)))
    ohalos = []
    for side, (start, to) in enumerate(((rows - EDGE, right), (0, left))):
        for j in range(peers):
            ohalos.append(remote(grad.at[pl.ds(start, EDGE)], ohalo.at[side, j], os_.at[side, j], or_.at[side, j], (to, tmate(j))))
    for copy in halos + ohalos:
        copy.start()
    pending += halos + ohalos
    chunks = gs.shape[1]
    step = rows // chunks

    def gather(j, r):
        at = pl.ds(pl.multiple_of(r * step, step), step)
        return remote(grad.at[at], others.at[j - 1, at], gs.at[j - 1, r], gr.at[j - 1, r], (sp, tmate(j)))

    for r in range(chunks):
        for j in range(1, peers):
            copy = gather(j, r)
            copy.start()
            pending.append(copy)

    matrix = group_matrix()
    gstep = divisor(rows, 256, 32)

    def own_gated(c):
        def chunk(r):
            at = pl.multiple_of(r * gstep, gstep)
            put_gated(gated, c, value[pl.ds(at, gstep), lanes(c)], gate[pl.ds(at, gstep), lanes(c)],
                      pl.multiple_of(at + wide, 8), gstep)

        loop(0, rows // gstep, chunk)

    loop(0, tiles, own_gated)
    for copy in halos:
        copy.wait_recv()
    inside = ((sp > 0).astype(F32), (sp < n - 1).astype(F32))

    def front(c):
        for side, dst in ((0, 0), (1, rows + wide)):
            put_gated(gated, c, vhalo[side, 0, :, lanes(c)].astype(F32) * inside[side],
                      vhalo[side, 1, :, lanes(c)], dst, wide)
        forward_tile(c, taps, gain, gated, unit, inv, normed, matrix)

    loop(0, tiles, front)

    def owner(j):
        return pl.ds(pl.multiple_of(lax.rem(tp + j, peers) * chans, chans), chans)

    per = wpart.shape[1]
    piece = max(divisor(chans, 256, 128), per)

    def weight_part(j):
        def cols(q):
            at = pl.ds(pl.multiple_of(q * piece, piece), piece)
            lhs = grad[:, at] if j == 0 else others[j - 1, :, at]
            out = lax.dot_general(lhs, normed[...], (((0,), (0,)), ((), ())), preferred_element_type=F32)
            base = lax.rem(tp + j, peers) * (chans // per) + q * (piece // per)
            wpart[pl.ds(base, piece // per)] = out.reshape(piece // per, per, chans)

        loop(0, chans // piece, cols)

    weight_part(0)
    gain_part[...] = jnp.zeros_like(gain_part)
    for copy in ohalos:
        copy.wait_recv()
    for side, at in ((0, 0), (1, rows + EDGE)):
        ng = sum(jnp.dot(ohalo[side, j], weight[owner(j), :], preferred_element_type=F32) for j in range(peers))
        act_to_conv(ng * inside[side], at, EDGE, False, unit, inv, gain, dconv, gain_part, matrix)

    def middle(r):
        at = pl.multiple_of(r * step, step)
        ng = jnp.dot(grad[pl.ds(at, step), :], weight[owner(0), :], preferred_element_type=F32)
        for j in range(1, peers):
            gather(j, r).wait_recv()
            ng += jnp.dot(others[j - 1, pl.ds(at, step), :], weight[owner(j), :], preferred_element_type=F32)
        act_to_conv(ng, pl.multiple_of(at + EDGE, 8), step, True, unit, inv, gain, dconv, gain_part, matrix)

    loop(0, chunks, middle)
    for j in range(1, peers):
        weight_part(j)

    def cast1(a):
        send1[a] = wpart[2 * a + 1 - b0].astype(BF16)

    loop(0, n // 2, cast1)
    copy1 = remote(send1, recv1, ws.at[0], wr.at[0], (mate0, tp))
    copy1.start()
    loop(0, half_tiles, lambda c: taps_tile(c, dconv, gated, gain_part, sums))
    copy1.wait_recv()

    def cast2(a):
        other, mine = 2 * a + 1 - b1, 2 * a + b1
        send2[a] = (wpart[2 * other + b0] + recv1[other].astype(F32)).astype(BF16)
        wpart[2 * mine + b0] = wpart[2 * mine + b0] + recv1[mine].astype(F32)

    loop(0, n // 4, cast2)
    copy2 = remote(send2, recv2, ws.at[1], wr.at[1], (mate1, tp))
    copy2.start()
    loop(half_tiles, tiles, lambda c: taps_tile(c, dconv, gated, gain_part, sums))

    acopy1 = remote(sums.at[pl.ds((1 - b0) * half_tiles, half_tiles)], arecv1, as_.at[0], ar.at[0], (mate0, tp))
    acopy1.start()
    quarter = max(tiles // 4, 1)
    loop(0, quarter, lambda c: backward_tile(c, dconv, value, gate, taps, vgrad, ggrad))
    acopy1.wait_recv()
    asum[0] = sums[pl.ds(b0 * half_tiles, half_tiles)] + arecv1[...]
    acopy2 = remote(asum.at[0], arecv2, as_.at[1], ar.at[1], (mate1, tp))
    acopy2.start()
    copy2.wait_recv()

    def total2(z):
        return wpart[4 * z + 2 * b1 + b0] + recv2[z].astype(F32)

    copies3 = []
    for d in range(1, group):
        send3[d - 1] = total2(lax.rem(zz + d, group)).astype(BF16)
    for d in range(1, group):
        copy = remote(send3.at[d - 1], recv3.at[d - 1], ws3.at[d - 1], wr3.at[d - 1], (zmate(d), tp))
        copy.start()
        copies3.append(copy)
    loop(quarter, 2 * quarter, lambda c: backward_tile(c, dconv, value, gate, taps, vgrad, ggrad))
    acopy2.wait_recv()
    asum[1] = asum[0] + arecv2[...]
    acopies3 = []
    for d in range(1, group):
        copy = remote(asum.at[1], arecv3.at[zz], as3.at[d - 1], ar3.at[d - 1], (zmate(d), tp))
        copy.start()
        acopies3.append(copy)
    loop(2 * quarter, tiles, lambda c: backward_tile(c, dconv, value, gate, taps, vgrad, ggrad))
    for d in range(1, group):
        peer = lax.rem(zz + group - d, group)
        remote(asum.at[1], arecv3.at[peer], as3.at[d - 1], ar3.at[d - 1], (zmate(d), tp)).wait_recv()
    arecv3[zz] = asum[1]
    total = arecv3[0]
    for z in range(1, group):
        total += arecv3[z]
    atotal[b0] = total
    acopy4 = remote(atotal.at[b0], atotal.at[b0], as_.at[2], ar.at[2], (mate0, tp))
    acopy4.start()
    final = total2(zz)
    for d in range(1, group):
        copies3[d - 1].wait_recv()
        final += recv3[d - 1].astype(F32)
    wout[...] = final
    remote(atotal.at[1 - b0], atotal.at[1 - b0], as_.at[2], ar.at[2], (mate0, tp)).wait_recv()
    out_sums[...] = atotal[...].reshape(out_sums.shape)
    for copy in pending + [copy1, copy2, acopy1, acopy2, acopy4] + copies3 + acopies3:
        copy.wait_send()


def per_device(value, gate, conv_taps, norm_gain, point_weight, out_grad):
    rows, chans = value.shape
    kw = conv_taps.shape[0]
    tiles = chans // LANE
    n, peers = lax.axis_size("sp"), lax.axis_size("tp")
    extent = rows + 2 * EDGE
    full = point_weight.shape[0]
    per = full // n
    group = n // 4
    taps = conv_taps.astype(F32).reshape(kw, tiles, LANE).transpose(1, 0, 2)
    gain = norm_gain.reshape(1, chans)
    args = (value, gate, taps, gain, point_weight, out_grad)
    half = (tiles // 2, kw + 1, LANE)
    vmem, dma = pltpu.VMEM, pltpu.SemaphoreType.DMA
    chunks = 4
    outs = [((rows, chans), BF16), ((rows, chans), BF16), ((tiles, kw + 1, LANE), F32), ((per, chans), F32)]
    vgrad, ggrad, sums, wgrad = pl.pallas_call(
        functools.partial(whole_kernel, n, peers),
        out_shape=[jax.ShapeDtypeStruct(s, d) for s, d in outs],
        in_specs=[pl.BlockSpec(memory_space=pltpu.VMEM)] * len(args),
        out_specs=[pl.BlockSpec(memory_space=pltpu.VMEM)] * len(outs),
        scratch_shapes=[
            vmem((tiles, rows + 4 * EDGE, LANE), F32),
            vmem((tiles, extent, LANE), F32),
            vmem((tiles, extent, LANE), F32),
            vmem((rows, chans), BF16),
            vmem((tiles, extent, LANE), F32),
            vmem((8, chans), F32),
            vmem((n, per, chans), F32),
            vmem((tiles, kw + 1, LANE), F32),
            vmem((2, 2, 2 * EDGE, chans), BF16),
            vmem((2, peers, EDGE, chans), BF16),
            vmem((peers - 1, rows, chans), BF16),
            vmem((n // 2, per, chans), BF16),
            vmem((n // 2, per, chans), BF16),
            vmem((n // 4, per, chans), BF16),
            vmem((n // 4, per, chans), BF16),
            vmem((group - 1, per, chans), BF16),
            vmem((group - 1, per, chans), BF16),
            vmem(half, F32),
            vmem(half, F32),
            vmem((2,) + half, F32),
            vmem((group,) + half, F32),
            vmem((2,) + half, F32),
            dma((2, 2)), dma((2, 2)), dma((2, peers)), dma((2, peers)),
            dma((peers - 1, chunks)), dma((peers - 1, chunks)),
            dma((2,)), dma((2,)), dma((group - 1,)), dma((group - 1,)),
            dma((3,)), dma((3,)), dma((group - 1,)), dma((group - 1,)),
        ],
        compiler_params=pltpu.CompilerParams(
            collective_id=0, has_side_effects=True, vmem_limit_bytes=56 * 1024 * 1024),
    )(*args)
    flat = sums.transpose(1, 0, 2).reshape(kw + 1, chans)
    return vgrad, ggrad, flat[:kw], flat[kw], wgrad


def solution(mesh):
    return jax.shard_map(
        per_device,
        mesh=mesh,
        in_specs=(P("sp", "tp"), P("sp", "tp"), P(None, "tp"), P("tp"), P(None, "tp"), P("sp", "tp")),
        out_specs=(P("sp", "tp"), P("sp", "tp"), P(None, "tp"), P("tp"), P("sp", "tp")),
        check_vma=False,
    )
```

```python
import functools

import jax
import jax.numpy as jnp
from jax import lax
from jax.experimental import pallas as pl
from jax.experimental.pallas import tpu as pltpu
from jax.sharding import PartitionSpec as P

GROUP = 64
EPS = 1e-06
LANE = 128
EDGE = 16
F32, BF16 = jnp.float32, jnp.bfloat16


def sigmoid(x):
    return 0.5 * jnp.tanh(0.5 * x) + 0.5


def divisor(total, *choices):
    for choice in choices:
        if total % choice == 0:
            return choice
    return total


def group_matrix():
    row = lax.broadcasted_iota(jnp.int32, (2 * LANE, LANE), 0)
    col = lax.broadcasted_iota(jnp.int32, (2 * LANE, LANE), 1)
    same = lax.rem(row, LANE) // GROUP == col // GROUP
    return jnp.where(same, 1.0 / GROUP, 0.0).astype(BF16)


def group_mean(x, matrix):
    high = x.astype(BF16)
    low = (x - high.astype(F32)).astype(BF16)
    return jnp.dot(jnp.concatenate([high, low], axis=1), matrix, preferred_element_type=F32)


def lanes(c):
    return pl.ds(pl.multiple_of(c * LANE, LANE), LANE)


def put_gated(gated, c, v, g, dst, n):
    gated[c, pl.ds(dst, n), :] = (v.astype(F32) * sigmoid(g.astype(F32))).astype(BF16).astype(F32)


def forward_tile(c, taps, gain, gated, unit, inv, normed, matrix):
    kw = taps.shape[1]
    extent = unit.shape[1]
    rows = normed.shape[0]
    cstep = divisor(extent, 96, 32)

    def conv(r, _):
        at = r * cstep
        acc = jnp.zeros((cstep, LANE), F32)
        for k in range(kw):
            acc += taps[c, pl.ds(k, 1), :] * gated[c, pl.ds(at + (k + EDGE - kw // 2), cstep), :]
        unit[c, pl.ds(pl.multiple_of(at, 8), cstep), :] = acc
        return 0

    lax.fori_loop(0, extent // cstep, conv, 0)
    nstep = divisor(extent, 352, 32)

    def norm(r, _):
        at = pl.multiple_of(r * nstep, 8)
        x = unit[c, pl.ds(at, nstep), :]
        centred = x - group_mean(x, matrix)
        rs = lax.rsqrt(group_mean(centred * centred, matrix) + EPS)
        inv[c, pl.ds(at, nstep), :] = rs
        unit[c, pl.ds(at, nstep), :] = centred * rs
        return 0

    lax.fori_loop(0, extent // nstep, norm, 0)
    step = divisor(rows, 256, 32)

    def act(r, _):
        at = pl.multiple_of(r * step, step)
        p = unit[c, pl.ds(pl.multiple_of(at + EDGE, 8), step), :] * gain[:, lanes(c)]
        normed[pl.ds(at, step), lanes(c)] = (p * sigmoid(p)).astype(BF16)
        return 0

    lax.fori_loop(0, rows // step, act, 0)


def act_to_conv(ng, at, n, own, unit, inv, gain, dconv, gain_part, matrix):
    for c in range(unit.shape[0]):
        g = gain[:, c * LANE:(c + 1) * LANE]
        u = unit[c, pl.ds(at, n), :]
        p = u * g
        s = sigmoid(p)
        a = ng[:, c * LANE:(c + 1) * LANE] * s * (1.0 + p * (1.0 - s))
        au = a * u
        if own:
            gain_part[:, c * LANE:(c + 1) * LANE] += jnp.sum(au.reshape(n // 8, 8, LANE), axis=0)
        h = a * g
        hu = au * g
        dconv[c, pl.ds(at, n), :] = inv[c, pl.ds(at, n), :] * (
            h - group_mean(h, matrix) - u * group_mean(hu, matrix))


def taps_tile(c, first, count, dconv, gated, tacc):
    kw = tacc.shape[1]

    def chunk(r, accs):
        at = first + r * 16
        out = []
        d0 = dconv[c, pl.ds(pl.multiple_of(at + EDGE, 8), 8), :]
        d1 = dconv[c, pl.ds(pl.multiple_of(at + EDGE + 8, 8), 8), :]
        for k in range(kw):
            g0 = gated[c, pl.ds(at + (k + 2 * EDGE - kw // 2), 8), :]
            g1 = gated[c, pl.ds(at + (k + 2 * EDGE - kw // 2 + 8), 8), :]
            out.append(accs[k] + (d0 * g0 + d1 * g1))
        return tuple(out)

    accs = lax.fori_loop(0, count // 16, chunk, tuple(tacc[c, k] for k in range(kw)))
    for k in range(kw):
        tacc[c, k] = accs[k]


def fold_taps(c, tacc, gain_part, sums):
    kw = tacc.shape[1]
    for k in range(kw):
        sums[c, pl.ds(k, 1), :] = jnp.sum(tacc[c, k], axis=0, keepdims=True)
    sums[c, pl.ds(kw, 1), :] = jnp.sum(gain_part[:, lanes(c)], axis=0, keepdims=True)


def backward_tile(c, dconv, value, gate, taps, vgrad, ggrad):
    rows = value.shape[0]
    kw = taps.shape[1]
    step = divisor(rows, 64, 32)

    def chunk(r, _):
        at = pl.multiple_of(r * step, step)
        acc = jnp.zeros((step, LANE), F32)
        for k in range(kw):
            acc += taps[c, pl.ds(k, 1), :] * dconv[c, pl.ds(at + (EDGE + kw // 2 - k), step), :]
        s = sigmoid(gate[pl.ds(at, step), lanes(c)].astype(F32))
        v = value[pl.ds(at, step), lanes(c)].astype(F32)
        gs = acc * s
        vgrad[pl.ds(at, step), lanes(c)] = gs.astype(BF16)
        ggrad[pl.ds(at, step), lanes(c)] = (gs * v * (1.0 - s)).astype(BF16)
        return 0

    lax.fori_loop(0, rows // step, chunk, 0)


def loop(lo, hi, body):
    def one(i, _):
        body(i)
        return 0

    lax.fori_loop(lo, hi, one, 0)


def whole_kernel(n, peers, value_in, gate_in, conv_taps, gain, weight_in, grad_in,
                 vgrad_out, ggrad_out, taps_out, gain_out, wout,
                 value, gate, weight, grad, vgrad, ggrad, taps, tacc, lsem, osem,
                 gated, unit, inv, normed, dconv, gain_part, wpart, sums,
                 vhalo, ohalo, others, send1, recv1, send2, recv2, send3, recv3,
                 arecv1, arecv2, asum, arecv3, atotal,
                 vs, vr, os_, or_, gs, gr, ws, wr, ws3, wr3, as_, ar, as3, ar3):
    rows, chans = value.shape
    tiles = chans // LANE
    sp, tp = lax.axis_index("sp"), lax.axis_index("tp")
    group = recv3.shape[0] + 1
    half_tiles = tiles // 2
    b0, b1, zz = lax.rem(sp, 2), lax.rem(sp // 2, 2), sp // 4
    left, right = lax.rem(sp + n - 1, n), lax.rem(sp + 1, n)
    mate0 = sp + 1 - 2 * b0
    mate1 = sp + 2 - 4 * b1

    def zmate(d):
        return lax.rem(sp + 4 * d, n)

    def tmate(j):
        return lax.rem(tp + peers - j, peers)

    def remote(src, dst, s, r, to):
        return pltpu.make_async_remote_copy(
            src_ref=src, dst_ref=dst, send_sem=s, recv_sem=r, device_id=to,
            device_id_type=pl.DeviceIdType.MESH)

    loads = [pltpu.make_async_copy(src, dst, lsem.at[i]) for i, (src, dst) in enumerate(
        ((value_in, value), (gate_in, gate), (grad_in, grad), (weight_in, weight)))]
    for copy in loads:
        copy.start()
    barrier = pltpu.get_barrier_semaphore()
    friends = [(left, tmate(j)) for j in range(peers)] + [(right, tmate(j)) for j in range(peers)]
    friends += [(sp, tmate(j)) for j in range(1, peers)] + [(mate0, tp), (mate1, tp)]
    friends += [(zmate(d), tp) for d in range(1, group)]
    for friend in friends:
        pl.semaphore_signal(barrier, inc=1, device_id=friend, device_id_type=pl.DeviceIdType.MESH)
    pl.semaphore_wait(barrier, len(friends))

    wide = 2 * EDGE
    pending = []
    halos = []
    for side, (start, to) in enumerate(((rows - wide, right), (0, left))):
        for i, ref in enumerate((value_in, gate_in)):
            halos.append(remote(ref.at[pl.ds(start, wide)], vhalo.at[side, i], vs.at[side, i], vr.at[side, i], (to, tp)))
    ohalos = []
    for side, (start, to) in enumerate(((rows - EDGE, right), (0, left))):
        for j in range(peers):
            ohalos.append(remote(grad_in.at[pl.ds(start, EDGE)], ohalo.at[side, j], os_.at[side, j], or_.at[side, j], (to, tmate(j))))
    for copy in halos + ohalos:
        copy.start()
    pending += halos + ohalos
    chunks = gs.shape[1]
    step = rows // chunks

    def gather(j, r):
        at = pl.ds(pl.multiple_of(r * step, step), step)
        return remote(grad_in.at[at], others.at[j - 1, at], gs.at[j - 1, r], gr.at[j - 1, r], (sp, tmate(j)))

    for r in range(chunks):
        for j in range(1, peers):
            copy = gather(j, r)
            copy.start()
            pending.append(copy)

    matrix = group_matrix()
    for c in range(tiles):
        taps[c] = conv_taps[:, c * LANE:(c + 1) * LANE].astype(F32)
    gain_part[...] = jnp.zeros_like(gain_part)
    tacc[...] = jnp.zeros_like(tacc)
    loads[0].wait()
    loads[1].wait()
    gstep = divisor(rows, 256, 32)

    def own_gated(c):
        def chunk(r):
            at = pl.multiple_of(r * gstep, gstep)
            put_gated(gated, c, value[pl.ds(at, gstep), lanes(c)], gate[pl.ds(at, gstep), lanes(c)],
                      pl.multiple_of(at + wide, 8), gstep)

        loop(0, rows // gstep, chunk)

    loop(0, tiles, own_gated)
    for copy in halos:
        copy.wait_recv()
    inside = ((sp > 0).astype(F32), (sp < n - 1).astype(F32))

    def front(c):
        for side, dst in ((0, 0), (1, rows + wide)):
            put_gated(gated, c, vhalo[side, 0, :, lanes(c)].astype(F32) * inside[side],
                      vhalo[side, 1, :, lanes(c)], dst, wide)
        forward_tile(c, taps, gain, gated, unit, inv, normed, matrix)

    loop(0, tiles, front)

    def owner(j):
        return pl.ds(pl.multiple_of(lax.rem(tp + j, peers) * chans, chans), chans)

    per = wpart.shape[1]
    piece = max(divisor(chans, 256, 128), per)

    def weight_part(j):
        def cols(q):
            at = pl.ds(pl.multiple_of(q * piece, piece), piece)
            lhs = grad[:, at] if j == 0 else others[j - 1, :, at]
            out = lax.dot_general(lhs, normed[...], (((0,), (0,)), ((), ())), preferred_element_type=F32)
            base = lax.rem(tp + j, peers) * (chans // per) + q * (piece // per)
            wpart[pl.ds(base, piece // per)] = out.reshape(piece // per, per, chans)

        loop(0, chans // piece, cols)

    pairs, quads = n // 2 // peers, n // 4 // peers
    span = group // peers

    def half1(j):
        at = pl.ds(lax.rem(tp + j, peers) * pairs, pairs)
        return remote(send1.at[at], recv1.at[at], ws.at[0, j], wr.at[0, j], (mate0, tp))

    def half2(j):
        at = pl.ds(lax.rem(tp + j, peers) * quads, quads)
        return remote(send2.at[at], recv2.at[at], ws.at[1, j], wr.at[1, j], (mate1, tp))

    def start1(j):
        first = lax.rem(tp + j, peers) * pairs

        def cast(i):
            send1[first + i] = wpart[2 * (first + i) + 1 - b0].astype(BF16)

        loop(0, pairs, cast)
        half1(j).start()

    def start2(j):
        first = lax.rem(tp + j, peers) * quads
        half1(j).wait_recv()

        def cast(i):
            other, mine = 2 * (first + i) + 1 - b1, 2 * (first + i) + b1
            send2[first + i] = (wpart[2 * other + b0] + recv1[other].astype(F32)).astype(BF16)
            wpart[2 * mine + b0] = wpart[2 * mine + b0] + recv1[mine].astype(F32)

        loop(0, quads, cast)
        half2(j).start()

    def total2(z):
        return wpart[4 * z + 2 * b1 + b0] + recv2[z].astype(F32)

    def final_copy(slot):
        return remote(send3.at[slot], recv3.at[slot], ws3.at[slot], wr3.at[slot],
                      (lax.rem(sp + 4 * (slot + 1), n), tp))

    def start3(j):
        half2(j).wait_recv()

        def one(i):
            z = lax.rem(tp + j, peers) * span + i
            d = lax.rem(z + group - zz, group)

            @pl.when(d != 0)
            def _():
                send3[d - 1] = total2(z).astype(BF16)
                final_copy(d - 1).start()

        loop(0, span, one)

    def await_chunk(r):
        for j in range(1, peers):
            gather(j, r).wait_recv()

    def middle(r):
        at = pl.multiple_of(r * step, step)
        ng = jnp.dot(grad[pl.ds(at, step), :], weight[owner(0), :], preferred_element_type=F32)
        for j in range(1, peers):
            ng += jnp.dot(others[j - 1, pl.ds(at, step), :], weight[owner(j), :], preferred_element_type=F32)
        act_to_conv(ng, pl.multiple_of(at + EDGE, 8), step, True, unit, inv, gain, dconv, gain_part, matrix)

    def taps_chunk(r):
        loop(0, tiles, lambda c: taps_tile(c, pl.multiple_of(r * step, step), step, dconv, gated, tacc))

    def both(r):
        await_chunk(r)
        middle(r)
        taps_chunk(r)

    def put_out(c):
        backward_tile(c, dconv, value, gate, taps, vgrad, ggrad)
        for copy in out_copies(c):
            copy.start()

    def out_copies(c):
        return (pltpu.make_async_copy(vgrad.at[:, lanes(c)], vgrad_out.at[:, lanes(c)], osem.at[0, c]),
                pltpu.make_async_copy(ggrad.at[:, lanes(c)], ggrad_out.at[:, lanes(c)], osem.at[1, c]))

    loads[2].wait()
    weight_part(0)
    start1(0)
    loads[3].wait()
    for copy in ohalos:
        copy.wait_recv()
    for side, at in ((0, 0), (1, rows + EDGE)):
        ng = sum(jnp.dot(ohalo[side, j], weight[owner(j), :], preferred_element_type=F32) for j in range(peers))
        act_to_conv(ng * inside[side], at, EDGE, False, unit, inv, gain, dconv, gain_part, matrix)
    start2(0)
    loop(0, chunks - 1, both)
    start3(0)
    await_chunk(chunks - 1)
    for j in range(1, peers):
        weight_part(j)
        start1(j)
    middle(chunks - 1)
    for j in range(1, peers):
        start2(j)
    taps_chunk(chunks - 1)
    loop(0, tiles, lambda c: fold_taps(c, tacc, gain_part, sums))

    acopy1 = remote(sums.at[pl.ds((1 - b0) * half_tiles, half_tiles)], arecv1, as_.at[0], ar.at[0], (mate0, tp))
    acopy1.start()
    quarter = max(tiles // 4, 1)
    loop(0, quarter, put_out)
    acopy1.wait_recv()
    asum[0] = sums[pl.ds(b0 * half_tiles, half_tiles)] + arecv1[...]
    acopy2 = remote(asum.at[0], arecv2, as_.at[1], ar.at[1], (mate1, tp))
    acopy2.start()
    loop(quarter, 2 * quarter, put_out)
    acopy2.wait_recv()
    asum[1] = asum[0] + arecv2[...]
    acopies3 = []
    for d in range(1, group):
        copy = remote(asum.at[1], arecv3.at[zz], as3.at[d - 1], ar3.at[d - 1], (zmate(d), tp))
        copy.start()
        acopies3.append(copy)
    for j in range(1, peers):
        start3(j)
    loop(2 * quarter, tiles, put_out)
    for d in range(1, group):
        peer = lax.rem(zz + group - d, group)
        remote(asum.at[1], arecv3.at[peer], as3.at[d - 1], ar3.at[d - 1], (zmate(d), tp)).wait_recv()
    arecv3[zz] = asum[1]
    total = arecv3[0]
    for z in range(1, group):
        total += arecv3[z]
    atotal[b0] = total
    acopy4 = remote(atotal.at[b0], atotal.at[b0], as_.at[2], ar.at[2], (mate0, tp))
    acopy4.start()
    final = total2(zz)
    for d in range(1, group):
        final_copy(d - 1).wait_recv()
        final += recv3[d - 1].astype(F32)
    wout[...] = final
    remote(atotal.at[1 - b0], atotal.at[1 - b0], as_.at[2], ar.at[2], (mate0, tp)).wait_recv()
    kw = tacc.shape[1]
    for c in range(tiles):
        tot = atotal[c // half_tiles, c % half_tiles]
        taps_out[:, c * LANE:(c + 1) * LANE] = tot[:kw]
        gain_out[:, c * LANE:(c + 1) * LANE] = tot[kw:]
    for copy in pending + [acopy1, acopy2, acopy4] + acopies3:
        copy.wait_send()
    for j in range(peers):
        half1(j).wait_send()
        half2(j).wait_send()
    for d in range(1, group):
        final_copy(d - 1).wait_send()

    def drain(c):
        for copy in out_copies(c):
            copy.wait()

    loop(0, tiles, drain)


def per_device(value, gate, conv_taps, norm_gain, point_weight, out_grad):
    rows, chans = value.shape
    kw = conv_taps.shape[0]
    tiles = chans // LANE
    n, peers = lax.axis_size("sp"), lax.axis_size("tp")
    extent = rows + 2 * EDGE
    full = point_weight.shape[0]
    per = full // n
    group = n // 4
    gain = norm_gain.reshape(1, chans)
    args = (value, gate, conv_taps, gain, point_weight, out_grad)
    half = (tiles // 2, kw + 1, LANE)
    vmem, dma = pltpu.VMEM, pltpu.SemaphoreType.DMA
    chunks = 4
    outs = [((rows, chans), BF16), ((rows, chans), BF16), ((kw, chans), F32), ((1, chans), F32), ((per, chans), F32)]
    vgrad, ggrad, taps_grad, gain_grad, wgrad = pl.pallas_call(
        functools.partial(whole_kernel, n, peers),
        out_shape=[jax.ShapeDtypeStruct(s, d) for s, d in outs],
        in_specs=[pl.BlockSpec(memory_space=m) for m in (pl.ANY, pl.ANY, vmem, vmem, pl.ANY, pl.ANY)],
        out_specs=[pl.BlockSpec(memory_space=m) for m in (pl.ANY, pl.ANY, vmem, vmem, vmem)],
        scratch_shapes=[
            vmem((rows, chans), BF16), vmem((rows, chans), BF16), vmem((full, chans), BF16), vmem((rows, chans), BF16),
            vmem((rows, chans), BF16), vmem((rows, chans), BF16),
            vmem((tiles, kw, LANE), F32),
            vmem((tiles, kw, 8, LANE), F32),
            dma((4,)), dma((2, tiles)),
            vmem((tiles, rows + 4 * EDGE, LANE), F32),
            vmem((tiles, extent, LANE), F32),
            vmem((tiles, extent, LANE), F32),
            vmem((rows, chans), BF16),
            vmem((tiles, extent, LANE), F32),
            vmem((8, chans), F32),
            vmem((n, per, chans), F32),
            vmem((tiles, kw + 1, LANE), F32),
            vmem((2, 2, 2 * EDGE, chans), BF16),
            vmem((2, peers, EDGE, chans), BF16),
            vmem((peers - 1, rows, chans), BF16),
            vmem((n // 2, per, chans), BF16),
            vmem((n // 2, per, chans), BF16),
            vmem((n // 4, per, chans), BF16),
            vmem((n // 4, per, chans), BF16),
            vmem((group - 1, per, chans), BF16),
            vmem((group - 1, per, chans), BF16),
            vmem(half, F32),
            vmem(half, F32),
            vmem((2,) + half, F32),
            vmem((group,) + half, F32),
            vmem((2,) + half, F32),
            dma((2, 2)), dma((2, 2)), dma((2, peers)), dma((2, peers)),
            dma((peers - 1, chunks)), dma((peers - 1, chunks)),
            dma((2, peers)), dma((2, peers)), dma((group - 1,)), dma((group - 1,)),
            dma((3,)), dma((3,)), dma((group - 1,)), dma((group - 1,)),
        ],
        compiler_params=pltpu.CompilerParams(
            collective_id=0, has_side_effects=True, vmem_limit_bytes=56 * 1024 * 1024),
    )(*args)
    return vgrad, ggrad, taps_grad, gain_grad.reshape(chans), wgrad


def solution(mesh):
    return jax.shard_map(
        per_device,
        mesh=mesh,
        in_specs=(P("sp", "tp"), P("sp", "tp"), P(None, "tp"), P("tp"), P(None, "tp"), P("sp", "tp")),
        out_specs=(P("sp", "tp"), P("sp", "tp"), P(None, "tp"), P("tp"), P("sp", "tp")),
        check_vma=False,
    )
```

```python
import functools

import jax
import jax.numpy as jnp
from jax import lax
from jax.experimental import pallas as pl
from jax.experimental.pallas import tpu as pltpu
from jax.sharding import PartitionSpec as P

GROUP = 64
EPS = 1e-06
LANE = 128
EDGE = 16
F32, BF16 = jnp.float32, jnp.bfloat16


def sigmoid(x):
    return 0.5 * jnp.tanh(0.5 * x) + 0.5


def divisor(total, *choices):
    for choice in choices:
        if total % choice == 0:
            return choice
    return total


def group_matrix():
    row = lax.broadcasted_iota(jnp.int32, (2 * LANE, LANE), 0)
    col = lax.broadcasted_iota(jnp.int32, (2 * LANE, LANE), 1)
    same = lax.rem(row, LANE) // GROUP == col // GROUP
    return jnp.where(same, 1.0 / GROUP, 0.0).astype(BF16)


def group_mean(x, matrix):
    high = x.astype(BF16)
    low = (x - high.astype(F32)).astype(BF16)
    return jnp.dot(jnp.concatenate([high, low], axis=1), matrix, preferred_element_type=F32)


def near_mean(x, matrix):
    return jnp.dot(x.astype(BF16), matrix[:LANE], preferred_element_type=F32)


def lanes(c):
    return pl.ds(pl.multiple_of(c * LANE, LANE), LANE)


def put_gated(gated, c, v, g, dst, n):
    gated[c, pl.ds(dst, n), :] = (v.astype(F32) * sigmoid(g.astype(F32))).astype(BF16).astype(F32)


def forward_tile(c, taps, gain, gated, unit, inv, normed, matrix):
    kw = taps.shape[1]
    extent = unit.shape[1]
    rows = normed.shape[0]
    cstep = divisor(extent, 96, 32)

    def conv(r, _):
        at = r * cstep
        acc = jnp.zeros((cstep, LANE), F32)
        for k in range(kw):
            acc += taps[c, pl.ds(k, 1), :] * gated[c, pl.ds(at + (k + EDGE - kw // 2), cstep), :]
        unit[c, pl.ds(pl.multiple_of(at, 8), cstep), :] = acc
        return 0

    lax.fori_loop(0, extent // cstep, conv, 0)
    nstep = divisor(extent, 352, 32)

    def norm(r, _):
        at = pl.multiple_of(r * nstep, 8)
        x = unit[c, pl.ds(at, nstep), :]
        centred = x - group_mean(x, matrix)
        rs = lax.rsqrt(near_mean(centred * centred, matrix) + EPS)
        inv[c, pl.ds(at, nstep), :] = rs
        unit[c, pl.ds(at, nstep), :] = centred * rs
        return 0

    lax.fori_loop(0, extent // nstep, norm, 0)
    step = divisor(rows, 256, 32)

    def act(r, _):
        at = pl.multiple_of(r * step, step)
        p = unit[c, pl.ds(pl.multiple_of(at + EDGE, 8), step), :] * gain[:, lanes(c)]
        normed[pl.ds(at, step), lanes(c)] = (p * sigmoid(p)).astype(BF16)
        return 0

    lax.fori_loop(0, rows // step, act, 0)


def act_to_conv(ng, at, n, own, unit, inv, gain, dconv, gain_part, matrix):
    for c in range(unit.shape[0]):
        g = gain[:, c * LANE:(c + 1) * LANE]
        u = unit[c, pl.ds(at, n), :]
        p = u * g
        s = sigmoid(p)
        a = ng[:, c * LANE:(c + 1) * LANE] * s * (1.0 + p * (1.0 - s))
        au = a * u
        if own:
            gain_part[:, c * LANE:(c + 1) * LANE] += jnp.sum(au.reshape(n // 8, 8, LANE), axis=0)
        h = a * g
        hu = au * g
        dconv[c, pl.ds(at, n), :] = inv[c, pl.ds(at, n), :] * (
            h - near_mean(h, matrix) - u * near_mean(hu, matrix))


def taps_tile(c, first, count, dconv, gated, tacc):
    kw = tacc.shape[1]

    def chunk(r, accs):
        at = first + r * 16
        out = []
        d0 = dconv[c, pl.ds(pl.multiple_of(at + EDGE, 8), 8), :]
        d1 = dconv[c, pl.ds(pl.multiple_of(at + EDGE + 8, 8), 8), :]
        for k in range(kw):
            g0 = gated[c, pl.ds(at + (k + 2 * EDGE - kw // 2), 8), :]
            g1 = gated[c, pl.ds(at + (k + 2 * EDGE - kw // 2 + 8), 8), :]
            out.append(accs[k] + (d0 * g0 + d1 * g1))
        return tuple(out)

    accs = lax.fori_loop(0, count // 16, chunk, tuple(tacc[c, k] for k in range(kw)))
    for k in range(kw):
        tacc[c, k] = accs[k]


def fold_taps(c, tacc, gain_part, sums):
    kw = tacc.shape[1]
    for k in range(kw):
        sums[c, pl.ds(k, 1), :] = jnp.sum(tacc[c, k], axis=0, keepdims=True)
    sums[c, pl.ds(kw, 1), :] = jnp.sum(gain_part[:, lanes(c)], axis=0, keepdims=True)


def backward_tile(c, dconv, value, gate, taps, vgrad, ggrad):
    rows = value.shape[0]
    kw = taps.shape[1]
    step = divisor(rows, 64, 32)

    def chunk(r, _):
        at = pl.multiple_of(r * step, step)
        acc = jnp.zeros((step, LANE), F32)
        for k in range(kw):
            acc += taps[c, pl.ds(k, 1), :] * dconv[c, pl.ds(at + (EDGE + kw // 2 - k), step), :]
        s = sigmoid(gate[pl.ds(at, step), lanes(c)].astype(F32))
        v = value[pl.ds(at, step), lanes(c)].astype(F32)
        gs = acc * s
        vgrad[pl.ds(at, step), lanes(c)] = gs.astype(BF16)
        ggrad[pl.ds(at, step), lanes(c)] = (gs * v * (1.0 - s)).astype(BF16)
        return 0

    lax.fori_loop(0, rows // step, chunk, 0)


def loop(lo, hi, body):
    def one(i, _):
        body(i)
        return 0

    lax.fori_loop(lo, hi, one, 0)


def whole_kernel(n, peers, value_in, gate_in, conv_taps, gain, weight_in, grad_in,
                 vgrad_out, ggrad_out, taps_out, gain_out, wout,
                 value, gate, weight, grad, vgrad, ggrad, taps, tacc, lsem, osem,
                 gated, unit, inv, normed, dconv, gain_part, wpart, sums,
                 vhalo, ohalo, others, send1, recv1, send2, recv2, send3, recv3,
                 arecv1, arecv2, asum, arecv3, atotal,
                 vs, vr, os_, or_, gs, gr, ws, wr, ws3, wr3, as_, ar, as3, ar3):
    rows, chans = value.shape
    tiles = chans // LANE
    sp, tp = lax.axis_index("sp"), lax.axis_index("tp")
    group = recv3.shape[0] + 1
    half_tiles = tiles // 2
    b0, b1, zz = lax.rem(sp, 2), lax.rem(sp // 2, 2), sp // 4
    left, right = lax.rem(sp + n - 1, n), lax.rem(sp + 1, n)
    mate0 = sp + 1 - 2 * b0
    mate1 = sp + 2 - 4 * b1

    def zmate(d):
        return lax.rem(sp + 4 * d, n)

    def tmate(j):
        return lax.rem(tp + peers - j, peers)

    def remote(src, dst, s, r, to):
        return pltpu.make_async_remote_copy(
            src_ref=src, dst_ref=dst, send_sem=s, recv_sem=r, device_id=to,
            device_id_type=pl.DeviceIdType.MESH)

    loads = [pltpu.make_async_copy(src, dst, lsem.at[i]) for i, (src, dst) in enumerate(
        ((value_in, value), (gate_in, gate), (grad_in, grad), (weight_in, weight)))]
    for copy in loads:
        copy.start()
    barrier = pltpu.get_barrier_semaphore()
    friends = [(left, tmate(j)) for j in range(peers)] + [(right, tmate(j)) for j in range(peers)]
    friends += [(sp, tmate(j)) for j in range(1, peers)] + [(mate0, tp), (mate1, tp)]
    friends += [(zmate(d), tp) for d in range(1, group)]
    for friend in friends:
        pl.semaphore_signal(barrier, inc=1, device_id=friend, device_id_type=pl.DeviceIdType.MESH)
    pl.semaphore_wait(barrier, len(friends))

    wide = 2 * EDGE
    pending = []
    halos = []
    for side, (start, to) in enumerate(((rows - wide, right), (0, left))):
        for i, ref in enumerate((value_in, gate_in)):
            halos.append(remote(ref.at[pl.ds(start, wide)], vhalo.at[side, i], vs.at[side, i], vr.at[side, i], (to, tp)))
    ohalos = []
    for side, (start, to) in enumerate(((rows - EDGE, right), (0, left))):
        for j in range(peers):
            ohalos.append(remote(grad_in.at[pl.ds(start, EDGE)], ohalo.at[side, j], os_.at[side, j], or_.at[side, j], (to, tmate(j))))
    for copy in halos + ohalos:
        copy.start()
    pending += halos + ohalos
    chunks = gs.shape[1]
    step = rows // chunks

    def gather(j, r):
        at = pl.ds(pl.multiple_of(r * step, step), step)
        return remote(grad_in.at[at], others.at[j - 1, at], gs.at[j - 1, r], gr.at[j - 1, r], (sp, tmate(j)))

    for r in range(chunks):
        for j in range(1, peers):
            copy = gather(j, r)
            copy.start()
            pending.append(copy)

    matrix = group_matrix()
    for c in range(tiles):
        taps[c] = conv_taps[:, c * LANE:(c + 1) * LANE].astype(F32)
    gain_part[...] = jnp.zeros_like(gain_part)
    tacc[...] = jnp.zeros_like(tacc)
    loads[0].wait()
    loads[1].wait()
    gstep = divisor(rows, 256, 32)

    def own_gated(c):
        def chunk(r):
            at = pl.multiple_of(r * gstep, gstep)
            put_gated(gated, c, value[pl.ds(at, gstep), lanes(c)], gate[pl.ds(at, gstep), lanes(c)],
                      pl.multiple_of(at + wide, 8), gstep)

        loop(0, rows // gstep, chunk)

    loop(0, tiles, own_gated)
    for copy in halos:
        copy.wait_recv()
    inside = ((sp > 0).astype(F32), (sp < n - 1).astype(F32))

    def front(c):
        for side, dst in ((0, 0), (1, rows + wide)):
            put_gated(gated, c, vhalo[side, 0, :, lanes(c)].astype(F32) * inside[side],
                      vhalo[side, 1, :, lanes(c)], dst, wide)
        forward_tile(c, taps, gain, gated, unit, inv, normed, matrix)

    loop(0, tiles, front)

    def owner(j):
        return pl.ds(pl.multiple_of(lax.rem(tp + j, peers) * chans, chans), chans)

    per = wpart.shape[1]
    piece = max(divisor(chans, 256, 128), per)

    def weight_part(j):
        def cols(q):
            at = pl.ds(pl.multiple_of(q * piece, piece), piece)
            lhs = grad[:, at] if j == 0 else others[j - 1, :, at]
            out = lax.dot_general(lhs, normed[...], (((0,), (0,)), ((), ())), preferred_element_type=F32)
            base = lax.rem(tp + j, peers) * (chans // per) + q * (piece // per)
            wpart[pl.ds(base, piece // per)] = out.reshape(piece // per, per, chans)

        loop(0, chans // piece, cols)

    pairs, quads = n // 2 // peers, n // 4 // peers
    span = group // peers

    def half1(j):
        at = pl.ds(lax.rem(tp + j, peers) * pairs, pairs)
        return remote(send1.at[at], recv1.at[at], ws.at[0, j], wr.at[0, j], (mate0, tp))

    def half2(j):
        at = pl.ds(lax.rem(tp + j, peers) * quads, quads)
        return remote(send2.at[at], recv2.at[at], ws.at[1, j], wr.at[1, j], (mate1, tp))

    def start1(j):
        first = lax.rem(tp + j, peers) * pairs

        def cast(i):
            send1[first + i] = wpart[2 * (first + i) + 1 - b0].astype(BF16)

        loop(0, pairs, cast)
        half1(j).start()

    def start2(j):
        first = lax.rem(tp + j, peers) * quads
        half1(j).wait_recv()

        def cast(i):
            other, mine = 2 * (first + i) + 1 - b1, 2 * (first + i) + b1
            send2[first + i] = (wpart[2 * other + b0] + recv1[other].astype(F32)).astype(BF16)
            wpart[2 * mine + b0] = wpart[2 * mine + b0] + recv1[mine].astype(F32)

        loop(0, quads, cast)
        half2(j).start()

    def total2(z):
        return wpart[4 * z + 2 * b1 + b0] + recv2[z].astype(F32)

    def final_copy(slot):
        return remote(send3.at[slot], recv3.at[slot], ws3.at[slot], wr3.at[slot],
                      (lax.rem(sp + 4 * (slot + 1), n), tp))

    def start3(j):
        half2(j).wait_recv()

        def one(i):
            z = lax.rem(tp + j, peers) * span + i
            d = lax.rem(z + group - zz, group)

            @pl.when(d != 0)
            def _():
                send3[d - 1] = total2(z).astype(BF16)
                final_copy(d - 1).start()

        loop(0, span, one)

    def await_chunk(r):
        for j in range(1, peers):
            gather(j, r).wait_recv()

    def middle(r):
        at = pl.multiple_of(r * step, step)
        ng = jnp.dot(grad[pl.ds(at, step), :], weight[owner(0), :], preferred_element_type=F32)
        for j in range(1, peers):
            ng += jnp.dot(others[j - 1, pl.ds(at, step), :], weight[owner(j), :], preferred_element_type=F32)
        act_to_conv(ng, pl.multiple_of(at + EDGE, 8), step, True, unit, inv, gain, dconv, gain_part, matrix)

    def taps_chunk(r):
        loop(0, tiles, lambda c: taps_tile(c, pl.multiple_of(r * step, step), step, dconv, gated, tacc))

    def both(r):
        await_chunk(r)
        middle(r)
        taps_chunk(r)

    def put_out(c):
        backward_tile(c, dconv, value, gate, taps, vgrad, ggrad)
        for copy in out_copies(c):
            copy.start()

    def out_copies(c):
        return (pltpu.make_async_copy(vgrad.at[:, lanes(c)], vgrad_out.at[:, lanes(c)], osem.at[0, c]),
                pltpu.make_async_copy(ggrad.at[:, lanes(c)], ggrad_out.at[:, lanes(c)], osem.at[1, c]))

    loads[2].wait()
    weight_part(0)
    start1(0)
    loads[3].wait()
    for copy in ohalos:
        copy.wait_recv()
    for side, at in ((0, 0), (1, rows + EDGE)):
        ng = sum(jnp.dot(ohalo[side, j], weight[owner(j), :], preferred_element_type=F32) for j in range(peers))
        act_to_conv(ng * inside[side], at, EDGE, False, unit, inv, gain, dconv, gain_part, matrix)
    start2(0)
    loop(0, chunks - 1, both)
    start3(0)
    await_chunk(chunks - 1)
    for j in range(1, peers):
        weight_part(j)
        start1(j)
    middle(chunks - 1)
    for j in range(1, peers):
        start2(j)
    taps_chunk(chunks - 1)
    loop(0, tiles, lambda c: fold_taps(c, tacc, gain_part, sums))

    acopy1 = remote(sums.at[pl.ds((1 - b0) * half_tiles, half_tiles)], arecv1, as_.at[0], ar.at[0], (mate0, tp))
    acopy1.start()
    quarter = max(tiles // 4, 1)
    loop(0, quarter, put_out)
    acopy1.wait_recv()
    asum[0] = sums[pl.ds(b0 * half_tiles, half_tiles)] + arecv1[...]
    acopy2 = remote(asum.at[0], arecv2, as_.at[1], ar.at[1], (mate1, tp))
    acopy2.start()
    loop(quarter, 2 * quarter, put_out)
    acopy2.wait_recv()
    asum[1] = asum[0] + arecv2[...]
    acopies3 = []
    for d in range(1, group):
        copy = remote(asum.at[1], arecv3.at[zz], as3.at[d - 1], ar3.at[d - 1], (zmate(d), tp))
        copy.start()
        acopies3.append(copy)
    for j in range(1, peers):
        start3(j)
    loop(2 * quarter, tiles, put_out)
    for d in range(1, group):
        peer = lax.rem(zz + group - d, group)
        remote(asum.at[1], arecv3.at[peer], as3.at[d - 1], ar3.at[d - 1], (zmate(d), tp)).wait_recv()
    arecv3[zz] = asum[1]
    total = arecv3[0]
    for z in range(1, group):
        total += arecv3[z]
    atotal[b0] = total
    acopy4 = remote(atotal.at[b0], atotal.at[b0], as_.at[2], ar.at[2], (mate0, tp))
    acopy4.start()
    final = total2(zz)
    for d in range(1, group):
        final_copy(d - 1).wait_recv()
        final += recv3[d - 1].astype(F32)
    wout[...] = final
    remote(atotal.at[1 - b0], atotal.at[1 - b0], as_.at[2], ar.at[2], (mate0, tp)).wait_recv()
    kw = tacc.shape[1]
    for c in range(tiles):
        tot = atotal[c // half_tiles, c % half_tiles]
        taps_out[:, c * LANE:(c + 1) * LANE] = tot[:kw]
        gain_out[:, c * LANE:(c + 1) * LANE] = tot[kw:]
    for copy in pending + [acopy1, acopy2, acopy4] + acopies3:
        copy.wait_send()
    for j in range(peers):
        half1(j).wait_send()
        half2(j).wait_send()
    for d in range(1, group):
        final_copy(d - 1).wait_send()

    def drain(c):
        for copy in out_copies(c):
            copy.wait()

    loop(0, tiles, drain)


def finish_kernel(parts, *refs):
    count = len(parts)
    sources, targets, held = refs[:count], refs[count:2 * count], refs[2 * count:3 * count]
    isem, osem = refs[3 * count:]
    incoming, outgoing = [], []
    slot = 0
    for src, dst, buf, pieces in zip(sources, targets, held, parts):
        size = src.shape[0] // pieces
        for p in range(pieces):
            at = pl.ds(p * size, size)
            incoming.append(pltpu.make_async_copy(src.at[at], buf.at[at], isem.at[slot]))
            outgoing.append(pltpu.make_async_copy(buf.at[at], dst.at[at], osem.at[slot]))
            slot += 1
    for copy in incoming:
        copy.start()
    for copy, after in zip(incoming, outgoing):
        copy.wait()
        after.start()
    for copy in outgoing:
        copy.wait()


def finish(*arrays):
    parts = [4 if a.shape[0] % 128 == 0 else 1 for a in arrays]
    sems = pltpu.SemaphoreType.DMA((sum(parts),))
    return pl.pallas_call(
        functools.partial(finish_kernel, parts),
        out_shape=[jax.ShapeDtypeStruct(a.shape, a.dtype) for a in arrays],
        in_specs=[pl.BlockSpec(memory_space=pl.ANY)] * len(arrays),
        out_specs=[pl.BlockSpec(memory_space=pl.ANY)] * len(arrays),
        scratch_shapes=[pltpu.VMEM(a.shape, a.dtype) for a in arrays] + [sems, sems],
        compiler_params=pltpu.CompilerParams(vmem_limit_bytes=60 * 1024 * 1024),
    )(*arrays)


def per_device(value, gate, conv_taps, norm_gain, point_weight, out_grad):
    rows, chans = value.shape
    kw = conv_taps.shape[0]
    tiles = chans // LANE
    n, peers = lax.axis_size("sp"), lax.axis_size("tp")
    extent = rows + 2 * EDGE
    full = point_weight.shape[0]
    per = full // n
    group = n // 4
    gain = norm_gain.reshape(1, chans)
    args = (value, gate, conv_taps, gain, point_weight, out_grad)
    half = (tiles // 2, kw + 1, LANE)
    vmem, dma = pltpu.VMEM, pltpu.SemaphoreType.DMA
    chunks = 4
    outs = [((rows, chans), BF16), ((rows, chans), BF16), ((kw, chans), F32), ((1, chans), F32), ((per, chans), F32)]
    vgrad, ggrad, taps_grad, gain_grad, wgrad = pl.pallas_call(
        functools.partial(whole_kernel, n, peers),
        out_shape=[jax.ShapeDtypeStruct(s, d) for s, d in outs],
        in_specs=[pl.BlockSpec(memory_space=m) for m in (pl.ANY, pl.ANY, vmem, vmem, pl.ANY, pl.ANY)],
        out_specs=[pl.BlockSpec(memory_space=m) for m in (pl.ANY, pl.ANY, vmem, vmem, vmem)],
        scratch_shapes=[
            vmem((rows, chans), BF16), vmem((rows, chans), BF16), vmem((full, chans), BF16), vmem((rows, chans), BF16),
            vmem((rows, chans), BF16), vmem((rows, chans), BF16),
            vmem((tiles, kw, LANE), F32),
            vmem((tiles, kw, 8, LANE), F32),
            dma((4,)), dma((2, tiles)),
            vmem((tiles, rows + 4 * EDGE, LANE), F32),
            vmem((tiles, extent, LANE), F32),
            vmem((tiles, extent, LANE), F32),
            vmem((rows, chans), BF16),
            vmem((tiles, extent, LANE), F32),
            vmem((8, chans), F32),
            vmem((n, per, chans), F32),
            vmem((tiles, kw + 1, LANE), F32),
            vmem((2, 2, 2 * EDGE, chans), BF16),
            vmem((2, peers, EDGE, chans), BF16),
            vmem((peers - 1, rows, chans), BF16),
            vmem((n // 2, per, chans), BF16),
            vmem((n // 2, per, chans), BF16),
            vmem((n // 4, per, chans), BF16),
            vmem((n // 4, per, chans), BF16),
            vmem((group - 1, per, chans), BF16),
            vmem((group - 1, per, chans), BF16),
            vmem(half, F32),
            vmem(half, F32),
            vmem((2,) + half, F32),
            vmem((group,) + half, F32),
            vmem((2,) + half, F32),
            dma((2, 2)), dma((2, 2)), dma((2, peers)), dma((2, peers)),
            dma((peers - 1, chunks)), dma((peers - 1, chunks)),
            dma((2, peers)), dma((2, peers)), dma((group - 1,)), dma((group - 1,)),
            dma((3,)), dma((3,)), dma((group - 1,)), dma((group - 1,)),
        ],
        compiler_params=pltpu.CompilerParams(
            collective_id=0, has_side_effects=True, vmem_limit_bytes=56 * 1024 * 1024),
    )(*args)
    vgrad, ggrad, taps_grad, gain_grad, wgrad = finish(vgrad, ggrad, taps_grad, gain_grad, wgrad)
    return vgrad, ggrad, taps_grad, gain_grad.reshape(chans), wgrad


def solution(mesh):
    return jax.shard_map(
        per_device,
        mesh=mesh,
        in_specs=(P("sp", "tp"), P("sp", "tp"), P(None, "tp"), P("tp"), P(None, "tp"), P("sp", "tp")),
        out_specs=(P("sp", "tp"), P("sp", "tp"), P(None, "tp"), P("tp"), P("sp", "tp")),
        check_vma=False,
    )
```
